32 devices in a mesh: sp: 8 (over z, x), tp: 4 (over y, core).
Axes of the slice: x: 2, y: 2, z: 4, core: 2. Of those that a mesh axis runs over, the one named last changes fastest.
Arguments:
- tokens: bfloat16 [1536, 2048], P(('sp', 'tp')), may hold values from -54 to 54
- w_query: bfloat16 [2048, 2048], P(None, 'tp'), may hold values from -0.21875 to 0.21875
- w_key: bfloat16 [2048, 2048], P(None, 'tp'), may hold values from -0.125 to 0.125
- w_value: bfloat16 [2048, 2048], P(None, 'tp'), may hold values from -0.125 to 0.125
- w_out: bfloat16 [2048, 2048], P('tp'), may hold values from -0.125 to 0.125
- mix_weight: float32 [16], P('tp'), may hold values from 0.3 to 0.8
- out_gain: float32 [128], replicated, may hold values from 0.1 to 1.9
Outputs:
- mixed: bfloat16 [1536, 2048], P(('sp', 'tp'))
The draws below stay inside these ranges and needn't reach their ends.
All inputs are finite; a program needn't handle non-finite values.
Results may differ from the reference program's by a relative error of at most 0.018.
The reference program's roundings to bfloat16 on the way (of `queries`, `keys`, `values`, `weights` and `normed`) count: a program that leaves them out, or rounds other values in their place, can miss the bound.
Values may be sent and summed in bfloat16 or wider, within the bound.
No kernel may reach another device: no remote copies, remote signals or barrier semaphores. Data moves between devices by JAX's collectives and lax.ppermute only.
A program may use at most 192 MiB of HBM per device.

```python
import math
import jax
import jax.numpy as jnp
from jax import lax

D = 2048
HEADS = 16
HD = 64
VD = 128
TOKENS = 1536


def draw_tokens(key, part):
    key_noise = jax.random.fold_in(key, 11)
    key_dir = jax.random.fold_in(key, 12)
    noise = jax.random.truncated_normal(key_noise, -6.0, 6.0, (TOKENS, D), jnp.float32)
    direction = jax.random.truncated_normal(key_dir, -6.0, 6.0, (D,), jnp.float32)
    place = jnp.arange(TOKENS, dtype=jnp.float32) / TOKENS
    drift = jnp.cos(3.14159265 * place)
    result = noise + drift[:, None] * direction[None, :]
    return result.astype(jnp.bfloat16)


def level_of(rng, shape, pieces, least, high):
    def one(position, shards_of):
        draws = jax.random.uniform(jax.random.fold_in(jax.random.fold_in(rng, 6), position), (shards_of,), jnp.float32, least / len(pieces), high / len(pieces))
        return jnp.repeat(jnp.exp(draws), shape[position] // shards_of).reshape((-1,) + (1,) * (len(shape) - position - 1))

    loudness = one(*pieces[0])
    for cut in pieces[1:]:
        loudness = loudness * one(*cut)
    return loudness


def gaussian(own_key, dims, deviation, reach, shards=(), held_as=jnp.bfloat16):
    values = jax.random.normal(own_key, dims, jnp.float32) * deviation
    if len(shards) > 0:
        values = level_of(own_key, dims, shards, -0.22, 0.18) * values
    return jnp.clip(values, min=-reach, max=reach).astype(held_as)


def setup_inputs(seed: int = 0) -> dict:
    seeds = jax.random.split(jax.random.key(seed), 8)
    tokens = draw_tokens(jax.random.fold_in(seeds[7], 71), 0)
    w_query = gaussian(seeds[1], (D, HEADS * 2 * HD), (D // 3) ** -0.5, 0.21875, ((1, 4),))
    w_key = gaussian(seeds[2], (D, HEADS * 2 * HD), D ** -0.5, 0.125, ((1, 4),))
    w_value = gaussian(seeds[3], (D, HEADS * VD), D ** -0.5, 0.125, ((1, 4),))
    w_out = gaussian(seeds[4], (HEADS * VD, D), (HEADS * VD) ** -0.5, 0.125, ((0, 4),))
    mix_weight = jnp.clip(0.3 + 0.5 * jax.random.uniform(seeds[5], (HEADS,), jnp.float32) ** level_of(seeds[5], (HEADS,), ((0, 4),), -0.2, 0.2), 0.3, 0.8)
    out_gain = jnp.clip(1.0 + 0.18 * jax.random.normal(seeds[6], (VD,), jnp.float32), 0.1, 1.9)
    return dict(tokens=tokens, w_query=w_query, w_key=w_key, w_value=w_value, w_out=w_out, mix_weight=mix_weight, out_gain=out_gain)


def one_head(args):
    query_h, key_h, value_h, lam = args
    block = math.gcd(TOKENS, 1024)
    query_blocks = query_h.reshape(TOKENS // block, block, 2, HD)
    key_f = key_h.astype(jnp.float32)
    value_f = value_h.astype(jnp.float32)

    def per_block(query_b):
        scores = jnp.einsum('qmd,kmd->mqk', query_b.astype(jnp.float32), key_f) * HD ** (-0.5)
        top = lax.optimization_barrier(jnp.max(scores, axis=-1, keepdims=True))
        expw = jnp.exp(scores - top)
        total = lax.optimization_barrier(jnp.sum(expw, axis=-1))
        weights = expw.astype(jnp.bfloat16).astype(jnp.float32)
        accum = jnp.einsum('mqk,ke->mqe', weights, value_f)
        return accum[0] / total[0][:, None] - lam * accum[1] / total[1][:, None]
    return lax.map(per_block, query_blocks).reshape(TOKENS, VD)

def reference(tokens, w_query, w_key, w_value, w_out, mix_weight, out_gain):
    queries = jnp.dot(tokens, w_query, preferred_element_type=jnp.float32).astype(jnp.bfloat16)
    keys = jnp.dot(tokens, w_key, preferred_element_type=jnp.float32).astype(jnp.bfloat16)
    values = jnp.dot(tokens, w_value, preferred_element_type=jnp.float32).astype(jnp.bfloat16)
    query_h = queries.reshape(TOKENS, HEADS, 2, HD).transpose(1, 0, 2, 3)
    key_h = keys.reshape(TOKENS, HEADS, 2, HD).transpose(1, 0, 2, 3)
    value_h = values.reshape(TOKENS, HEADS, VD).transpose(1, 0, 2)
    heads_out = lax.map(one_head, (query_h, key_h, value_h, mix_weight))
    meansq = lax.optimization_barrier(jnp.mean(heads_out * heads_out, axis=-1, keepdims=True))
    normed = (heads_out * lax.rsqrt(meansq + 1e-06) * out_gain).astype(jnp.bfloat16)
    normed = normed.transpose(1, 0, 2).reshape(TOKENS, HEADS * VD)
    return jnp.dot(normed, w_out, preferred_element_type=jnp.float32).astype(jnp.bfloat16)
```

```python
import jax
import jax.numpy as jnp
from jax import lax
from jax.experimental import pallas as pl
from jax.experimental.pallas import tpu as pltpu
from jax.sharding import PartitionSpec as P

VMEM = pl.BlockSpec(memory_space=pltpu.VMEM)
SMEM = pl.BlockSpec(memory_space=pltpu.SMEM)
F32 = jnp.float32
BF16 = jnp.bfloat16
LOG2E = 1.4426950408889634


def swap(array, axis, size, mask):
    return lax.ppermute(array, axis, [(i, i ^ mask) for i in range(size)])


def project(blocks, w_query, w_key, w_value, head, heads, shared):
    rows = sum(b.shape[0] for b in blocks)
    qk = w_query.shape[1] // heads
    vd = w_value.shape[1] // heads
    n = len(blocks)

    def body(head_ref, *refs):
        ins, (wq, wk, wv), outs, (sq, sk, sv) = refs[:n], refs[n : n + 3], refs[n + 3 : -3], refs[-3:]
        x = jnp.concatenate([r[...] for r in ins], axis=0)
        for w, s in ((wk, sk), (wv, sv), (wq, sq)):
            s[...] = jnp.dot(x, w[...], preferred_element_type=F32).astype(BF16)
        for j in range(heads):
            h = head_ref[0] ^ j
            k = sk[:, pl.ds(pl.multiple_of(h * qk, qk), qk)]
            v = sv[:, pl.ds(pl.multiple_of(h * vd, vd), vd)]
            q = sq[:, pl.ds(pl.multiple_of(h * qk, qk), qk)]
            full = outs[j]
            full[:, :qk] = k
            full[:, qk : qk + vd] = v
            full[:, qk + vd :] = q
            if shared:
                outs[heads + j][:, :qk] = k
                outs[heads + j][:, qk:] = v

    shapes = [jax.ShapeDtypeStruct((rows, 2 * qk + vd), BF16)] * heads
    if shared:
        shapes += [jax.ShapeDtypeStruct((rows, qk + vd), BF16)] * heads
    return pl.pallas_call(
        body,
        out_shape=shapes,
        in_specs=[SMEM] + [VMEM] * (n + 3),
        out_specs=[VMEM] * len(shapes),
        scratch_shapes=[
            pltpu.VMEM((rows, w_query.shape[1]), BF16),
            pltpu.VMEM((rows, w_key.shape[1]), BF16),
            pltpu.VMEM((rows, w_value.shape[1]), BF16),
        ],
        name="project",
    )(head, *blocks, w_query, w_key, w_value)


def attend(q_parts, kv_parts, mix, gain, head, qk, vd):
    nq = len(q_parts)
    rows = q_parts[0].shape[0]
    parts = list(q_parts) + list(kv_parts)
    n = len(parts)
    queries, keys = nq * rows, n * rows
    half = qk // 2
    block = 256 if queries % 256 == 0 else rows
    chunk = max(c * rows for c in range(1, n + 1) if n % c == 0 and c * rows <= 2048)
    factor = half**-0.5 * LOG2E

    def body(head_ref, mix_ref, gain_ref, *refs):
        ins, outs, (sk, sv, sq, so) = refs[:n], refs[n : n + nq], refs[n + nq :]
        for i, r in enumerate(ins):
            at = i * rows
            sk[at : at + rows, :] = r[:, :qk]
            c, o = divmod(at, chunk)
            sv[c, :, o : o + rows] = r[:, qk : qk + vd].astype(F32).T.astype(BF16)
            if i < nq:
                sq[at : at + rows, :] = r[:, qk + vd :]
        lam = mix_ref[head_ref[0]]
        lane = lax.broadcasted_iota(jnp.int32, (block, qk), 1)

        def piece(q, c):
            at = c * chunk if isinstance(c, int) else pl.multiple_of(c * chunk, rows)
            s = lax.dot_general(
                sk[pl.ds(at, chunk), :], q, (((1,), (1,)), ((), ())), preferred_element_type=F32
            )
            return s, jnp.max(s, axis=0, keepdims=True)

        def softmax(q):
            if keys == chunk:
                s, top = piece(q, 0)
                e = jnp.exp2((s - top) * factor)
                acc = jnp.dot(sv[0], e.astype(BF16), preferred_element_type=F32)
                return acc / jnp.sum(e, axis=0, keepdims=True)

            def step(c, carry):
                old, total, acc = carry
                s, top = piece(q, c)
                top = jnp.maximum(old, top)
                fix = jnp.exp2((old - top) * factor)
                e = jnp.exp2((s - top) * factor)
                acc = acc * fix + jnp.dot(sv[c], e.astype(BF16), preferred_element_type=F32)
                return top, total * fix + jnp.sum(e, axis=0, keepdims=True), acc

            start = (
                jnp.full((1, block), -1e30, F32),
                jnp.zeros((1, block), F32),
                jnp.zeros((vd, block), F32),
            )
            top, total, acc = lax.fori_loop(0, keys // chunk, step, start)
            return acc / total

        for b in range(queries // block):
            q = sq[b * block : (b + 1) * block, :]
            zero = jnp.zeros_like(q)
            first = softmax(jnp.where(lane < half, q, zero))
            second = softmax(jnp.where(lane < half, zero, q))
            ho = first - lam * second
            ho = ho * lax.rsqrt(jnp.mean(ho * ho, axis=0, keepdims=True) + 1e-06)
            so[b * block : (b + 1) * block, :] = (ho.T * gain_ref[...]).astype(BF16)
        for i in range(nq):
            outs[i][...] = so[i * rows : (i + 1) * rows, :]

    return pl.pallas_call(
        body,
        out_shape=[jax.ShapeDtypeStruct((rows, vd), BF16)] * nq,
        in_specs=[SMEM, SMEM] + [VMEM] * (n + 1),
        out_specs=[VMEM] * nq,
        scratch_shapes=[
            pltpu.VMEM((keys, qk), BF16),
            pltpu.VMEM((keys // chunk, vd, chunk), BF16),
            pltpu.VMEM((queries, qk), BF16),
            pltpu.VMEM((queries, vd), BF16),
        ],
        name="attend",
    )(head, mix, gain.reshape(1, vd), *parts)


def project_out(normed, w_out, head, masks, rows):
    heads = len(normed)
    total, vd = normed[0].shape

    def body(head_ref, *refs):
        ins, w, outs, sx = refs[:heads], refs[heads], refs[heads + 1 : -1], refs[-1]
        for j in range(heads):
            h = head_ref[0] ^ j
            sx[:, pl.ds(pl.multiple_of(h * vd, vd), vd)] = ins[j][...]
        y = jnp.dot(sx[...], w[...], preferred_element_type=F32)
        for i in range(len(masks)):
            outs[i][...] = y[i * rows : (i + 1) * rows].astype(BF16)

    return pl.pallas_call(
        body,
        out_shape=[jax.ShapeDtypeStruct((rows, w_out.shape[1]), BF16)] * len(masks),
        in_specs=[SMEM] + [VMEM] * (heads + 1),
        out_specs=[VMEM] * len(masks),
        scratch_shapes=[pltpu.VMEM((total, heads * vd), BF16)],
        name="project_out",
    )(head, *normed, w_out)


def make(n_sp, n_tp):
    def shards(tokens, w_query, w_key, w_value, w_out, mix_weight, out_gain):
        heads = mix_weight.shape[0]
        qk = w_query.shape[1] // heads
        vd = w_value.shape[1] // heads
        rows = tokens.shape[0]
        sharing = n_sp // heads
        head = (lax.axis_index("sp") // sharing).astype(jnp.int32).reshape(1)

        bits = []
        while (1 << len(bits)) < n_tp:
            bits.append(1 << len(bits))
        masks, blocks = [0], [tokens]
        for bit in reversed(bits):
            blocks = blocks + [swap(b, "tp", n_tp, bit) for b in blocks]
            masks = masks + [m | bit for m in masks]

        mine = project(blocks, w_query, w_key, w_value, head, heads, sharing > 1)
        q_parts, kv_parts = [], []
        for j in range(heads):
            for r in range(sharing):
                mask = j * sharing + r
                if r:
                    kv_parts.append(swap(mine[heads + j], "sp", n_sp, mask))
                else:
                    q_parts.append(swap(mine[j], "sp", n_sp, mask) if mask else mine[j])
        out = attend(q_parts, kv_parts, mix_weight, out_gain, head, qk, vd)
        normed = [out[0]] + [swap(out[j], "sp", n_sp, j * sharing) for j in range(1, heads)]
        parts = dict(zip(masks, project_out(normed, w_out, head, masks, rows)))
        for bit in bits:
            moved = {m: swap(p, "tp", n_tp, bit) for m, p in parts.items() if m & bit}
            parts = {
                m: (p.astype(F32) + moved[m | bit].astype(F32)).astype(BF16)
                for m, p in parts.items()
                if not m & bit
            }
        return parts[0]

    return shards


def solution(mesh):
    in_specs = (
        P(("sp", "tp"), None),
        P(None, "tp"),
        P(None, "tp"),
        P(None, "tp"),
        P("tp", None),
        P("tp"),
        P(),
    )
    out_specs = P(("sp", "tp"), None)
    body = make(mesh.shape["sp"], mesh.shape["tp"])
    return jax.shard_map(body, mesh=mesh, in_specs=in_specs, out_specs=out_specs, check_vma=False)
```

```python
import jax
import jax.numpy as jnp
from jax import lax
from jax.experimental import pallas as pl
from jax.experimental.pallas import tpu as pltpu
from jax.sharding import PartitionSpec as P


VMEM = pl.BlockSpec(memory_space=pltpu.VMEM)
SMEM = pl.BlockSpec(memory_space=pltpu.SMEM)
F32 = jnp.float32
BF16 = jnp.bfloat16
LOG2E = 1.4426950408889634


def swap(array, axis, size, mask):
    return lax.ppermute(array, axis, [(i, i ^ mask) for i in range(size)])


def project_own(x, weights):
    rows = x.shape[0]

    def body(x_ref, *refs):
        for w, o in zip(refs[:3], refs[3:]):
            o[...] = jnp.dot(x_ref[...], w[...], preferred_element_type=F32).astype(BF16)

    flops = sum(2 * rows * w.size for w in weights)
    return pl.pallas_call(
        body,
        out_shape=[jax.ShapeDtypeStruct((rows, w.shape[1]), BF16) for w in weights],
        in_specs=[VMEM] * 4,
        out_specs=[VMEM] * 3,
        cost_estimate=pl.CostEstimate(
            flops=8 * flops, bytes_accessed=sum(2 * w.size for w in weights), transcendentals=0
        ),
        compiler_params=pltpu.CompilerParams(vmem_limit_bytes=12 << 20),
        name="project_own",
    )(x, *weights)


def project(own, blocks, weights, heads, sharing):
    start = own[0].shape[0]
    rows = start + sum(b.shape[0] for b in blocks)
    widths = [w.shape[1] // heads for w in weights]
    n = len(blocks)

    def body(*refs):
        own_head = lax.axis_index("sp") // sharing
        firsts, ins, ws = refs[:3], refs[3 : n + 3], refs[n + 3 : n + 6]
        outs, res = refs[n + 6 : -3], refs[-3:]
        if n:
            x = jnp.concatenate([r[...] for r in ins], axis=0)
        at = 0
        for i, (f, w, s, width) in enumerate(zip(firsts, ws, res, widths)):
            s[:start, :] = f[...]
            if n:
                s[start:, :] = jnp.dot(x, w[...], preferred_element_type=F32).astype(BF16)
            for j in range(heads):
                h = own_head ^ j
                part = s[:, pl.ds(pl.multiple_of(h * width, width), width)]
                outs[j][:, at : at + width] = part
                if sharing > 1 and i < 2:
                    outs[heads + j][:, at : at + width] = part
            at += width

    shapes = [jax.ShapeDtypeStruct((rows, sum(widths)), BF16)] * heads
    if sharing > 1:
        shapes += [jax.ShapeDtypeStruct((rows, sum(widths[:2])), BF16)] * heads
    return pl.pallas_call(
        body,
        out_shape=shapes,
        in_specs=[VMEM] * (n + 6),
        out_specs=[VMEM] * len(shapes),
        scratch_shapes=[pltpu.VMEM((rows, w.shape[1]), BF16) for w in weights],
        compiler_params=pltpu.CompilerParams(vmem_limit_bytes=20 << 20),
        name="project",
    )(*own, *blocks, *weights)


def attend(q_parts, kv_parts, mix, gain, sharing, qk, vd):
    nq = len(q_parts)
    rows = q_parts[0].shape[0]
    parts = list(q_parts) + list(kv_parts)
    n = len(parts)
    queries, keys = nq * rows, n * rows
    half = qk // 2
    block = 256 if queries % 256 == 0 else rows
    chunk = max(c * rows for c in range(1, n + 1) if n % c == 0 and c * rows <= 2048)
    factor = half**-0.5 * LOG2E

    def body(mix_ref, gain_ref, *refs):
        own_head = lax.axis_index("sp") // sharing
        ins, outs, (sk, sv, sq, so) = refs[:n], refs[n : n + nq], refs[n + nq :]
        for i, r in enumerate(ins):
            at = i * rows
            sk[at : at + rows, :] = r[:, :qk]
            c, o = divmod(at, chunk)
            sv[c, :, o : o + rows] = r[:, qk : qk + vd].astype(F32).T.astype(BF16)
            if i < nq:
                sq[at : at + rows, :] = r[:, qk + vd :]
        lam = mix_ref[own_head]
        lane = lax.broadcasted_iota(jnp.int32, (block, qk), 1)

        def piece(q, c):
            at = c * chunk if isinstance(c, int) else pl.multiple_of(c * chunk, rows)
            s = lax.dot_general(
                sk[pl.ds(at, chunk), :], q, (((1,), (1,)), ((), ())), preferred_element_type=F32
            )
            return s, jnp.max(s, axis=0, keepdims=True)

        def softmax(q):
            if keys == chunk:
                s, top = piece(q, 0)
                e = jnp.exp2((s - top) * factor)
                acc = jnp.dot(sv[0], e.astype(BF16), preferred_element_type=F32)
                return acc / jnp.sum(e, axis=0, keepdims=True)

            def step(c, carry):
                old, total, acc = carry
                s, top = piece(q, c)
                top = jnp.maximum(old, top)
                fix = jnp.exp2((old - top) * factor)
                e = jnp.exp2((s - top) * factor)
                acc = acc * fix + jnp.dot(sv[c], e.astype(BF16), preferred_element_type=F32)
                return top, total * fix + jnp.sum(e, axis=0, keepdims=True), acc

            start = (
                jnp.full((1, block), -1e30, F32),
                jnp.zeros((1, block), F32),
                jnp.zeros((vd, block), F32),
            )
            top, total, acc = lax.fori_loop(0, keys // chunk, step, start)
            return acc / total

        for b in range(queries // block):
            q = sq[b * block : (b + 1) * block, :]
            zero = jnp.zeros_like(q)
            first = softmax(jnp.where(lane < half, q, zero))
            second = softmax(jnp.where(lane < half, zero, q))
            ho = first - lam * second
            ho = ho * lax.rsqrt(jnp.mean(ho * ho, axis=0, keepdims=True) + 1e-06)
            so[b * block : (b + 1) * block, :] = (ho.T * gain_ref[...]).astype(BF16)
        for i in range(nq):
            outs[i][...] = so[i * rows : (i + 1) * rows, :]

    return pl.pallas_call(
        body,
        out_shape=[jax.ShapeDtypeStruct((rows, vd), BF16)] * nq,
        in_specs=[SMEM] + [VMEM] * (n + 1),
        out_specs=[VMEM] * nq,
        scratch_shapes=[
            pltpu.VMEM((keys, qk), BF16),
            pltpu.VMEM((keys // chunk, vd, chunk), BF16),
            pltpu.VMEM((queries, qk), BF16),
            pltpu.VMEM((queries, vd), BF16),
        ],
        compiler_params=pltpu.CompilerParams(vmem_limit_bytes=24 << 20),
        name="attend",
    )(mix, gain.reshape(1, vd), *parts)


def project_out(normed, w_out, sharing, masks, rows):
    heads = len(normed)
    total, vd = normed[0].shape

    def body(*refs):
        own_head = lax.axis_index("sp") // sharing
        ins, w, outs, sx = refs[:heads], refs[heads], refs[heads + 1 : -1], refs[-1]
        for j in range(heads):
            h = own_head ^ j
            sx[:, pl.ds(pl.multiple_of(h * vd, vd), vd)] = ins[j][...]
        y = jnp.dot(sx[...], w[...], preferred_element_type=F32)
        for i in range(len(masks)):
            outs[i][...] = y[i * rows : (i + 1) * rows].astype(BF16)

    return pl.pallas_call(
        body,
        out_shape=[jax.ShapeDtypeStruct((rows, w_out.shape[1]), BF16)] * len(masks),
        in_specs=[VMEM] * (heads + 1),
        out_specs=[VMEM] * len(masks),
        scratch_shapes=[pltpu.VMEM((total, heads * vd), BF16)],
        compiler_params=pltpu.CompilerParams(vmem_limit_bytes=12 << 20),
        name="project_out",
    )(*normed, w_out)


def make(n_sp, n_tp):
    def shards(tokens, w_query, w_key, w_value, w_out, mix_weight, out_gain):
        heads = mix_weight.shape[0]
        qk = w_query.shape[1] // heads
        vd = w_value.shape[1] // heads
        rows = tokens.shape[0]
        sharing = n_sp // heads

        weights = (w_key, w_value, w_query)
        bits = []
        while (1 << len(bits)) < n_tp:
            bits.append(1 << len(bits))
        masks, blocks = [0], [tokens]
        for bit in reversed(bits):
            blocks = blocks + [swap(b, "tp", n_tp, bit) for b in blocks]
            masks = masks + [m | bit for m in masks]

        own = project_own(tokens, weights)
        mine = project(own, blocks[1:], weights, heads, sharing)
        q_parts = [mine[0]] + [None] * (heads - 1)
        kv_parts = {}
        relay = heads // 2
        order = ([relay] if relay else []) + [j for j in reversed(range(heads)) if j != relay]
        for j in order:
            if j:
                q_parts[j] = swap(mine[j], "sp", n_sp, j * sharing)
            if not (j and j == relay):
                for r in range(1, sharing):
                    kv_parts[j, r] = swap(mine[heads + j], "sp", n_sp, j * sharing + r)
        if relay:
            for r in range(1, sharing):
                kv_parts[relay, r] = swap(q_parts[relay], "sp", n_sp, r)
        kv_parts = list(kv_parts.values())
        out = attend(q_parts, kv_parts, mix_weight, out_gain, sharing, qk, vd)
        normed = [out[0]] + [swap(out[j], "sp", n_sp, j * sharing) for j in range(1, heads)]
        parts = dict(zip(masks, project_out(normed, w_out, sharing, masks, rows)))
        for bit in bits:
            moved = {m: swap(p, "tp", n_tp, bit) for m, p in parts.items() if m & bit}
            parts = {
                m: (p.astype(F32) + moved[m | bit].astype(F32)).astype(BF16)
                for m, p in parts.items()
                if not m & bit
            }
        return parts[0]

    return shards


def solution(mesh):
    in_specs = (
        P(("sp", "tp"), None),
        P(None, "tp"),
        P(None, "tp"),
        P(None, "tp"),
        P("tp", None),
        P("tp"),
        P(),
    )
    out_specs = P(("sp", "tp"), None)
    inner = make(mesh.shape["sp"], mesh.shape["tp"])

    return jax.shard_map(inner, mesh=mesh, in_specs=in_specs, out_specs=out_specs, check_vma=False)
```

```python
import jax
import jax.numpy as jnp
from jax import lax
from jax.experimental import pallas as pl
from jax.experimental.pallas import tpu as pltpu
from jax.sharding import PartitionSpec as P


VMEM = pl.BlockSpec(memory_space=pltpu.VMEM)
SMEM = pl.BlockSpec(memory_space=pltpu.SMEM)
F32 = jnp.float32
BF16 = jnp.bfloat16
LOG2E = 1.4426950408889634


def swap(array, axis, size, mask):
    return lax.ppermute(array, axis, [(i, i ^ mask) for i in range(size)])


def project_own(x, weights):
    rows = x.shape[0]

    def body(x_ref, *refs):
        for w, o in zip(refs[:3], refs[3:]):
            o[...] = jnp.dot(x_ref[...], w[...], preferred_element_type=F32).astype(BF16)

    flops = sum(2 * rows * w.size for w in weights)
    return pl.pallas_call(
        body,
        out_shape=[jax.ShapeDtypeStruct((rows, w.shape[1]), BF16) for w in weights],
        in_specs=[VMEM] * 4,
        out_specs=[VMEM] * 3,
        cost_estimate=pl.CostEstimate(
            flops=8 * flops, bytes_accessed=sum(2 * w.size for w in weights), transcendentals=0
        ),
        compiler_params=pltpu.CompilerParams(vmem_limit_bytes=12 << 20),
        name="project_own",
    )(x, *weights)


def project(own, blocks, weights, heads, sharing):
    start = own[0].shape[0]
    rows = start + sum(b.shape[0] for b in blocks)
    widths = [w.shape[1] // heads for w in weights]
    n = len(blocks)

    def body(*refs):
        own_head = lax.axis_index("sp") // sharing
        firsts, ins, ws = refs[:3], refs[3 : n + 3], refs[n + 3 : n + 6]
        outs, res = refs[n + 6 : -3], refs[-3:]
        if n:
            x = jnp.concatenate([r[...] for r in ins], axis=0)
        at = 0
        for i, (f, w, s, width) in enumerate(zip(firsts, ws, res, widths)):
            s[:start, :] = f[...]
            if n:
                s[start:, :] = jnp.dot(x, w[...], preferred_element_type=F32).astype(BF16)
            for j in range(heads):
                h = own_head ^ j
                part = s[:, pl.ds(pl.multiple_of(h * width, width), width)]
                outs[j][:, at : at + width] = part
                if sharing > 1 and i < 2:
                    outs[heads + j][:, at : at + width] = part
            at += width

    shapes = [jax.ShapeDtypeStruct((rows, sum(widths)), BF16)] * heads
    if sharing > 1:
        shapes += [jax.ShapeDtypeStruct((rows, sum(widths[:2])), BF16)] * heads
    return pl.pallas_call(
        body,
        out_shape=shapes,
        in_specs=[VMEM] * (n + 6),
        out_specs=[VMEM] * len(shapes),
        scratch_shapes=[pltpu.VMEM((rows, w.shape[1]), BF16) for w in weights],
        compiler_params=pltpu.CompilerParams(vmem_limit_bytes=20 << 20),
        name="project",
    )(*own, *blocks, *weights)


def attend(q_parts, kv_parts, mix, gain, sharing, qk, vd):
    nq = len(q_parts)
    rows = q_parts[0].shape[0]
    parts = list(q_parts) + list(kv_parts)
    n = len(parts)
    queries, keys = nq * rows, n * rows
    half = qk // 2
    block = next((b for b in (256, 384, 128) if queries % b == 0), rows)
    chunk = max(c * rows for c in range(1, n + 1) if n % c == 0 and c * rows <= 2048)
    factor = half**-0.5 * LOG2E

    def body(mix_ref, gain_ref, *refs):
        own_head = lax.axis_index("sp") // sharing
        ins, outs, (sk, sv, sq, so) = refs[:n], refs[n : n + nq], refs[n + nq :]
        for i, r in enumerate(ins):
            at = i * rows
            sk[at : at + rows, :] = r[:, :qk]
            c, o = divmod(at, chunk)
            sv[c, :, o : o + rows] = r[:, qk : qk + vd].astype(F32).T.astype(BF16)
            if i < nq:
                sq[at : at + rows, :] = r[:, qk + vd :]
        lam = mix_ref[own_head]
        lane = lax.broadcasted_iota(jnp.int32, (block, qk), 1)

        def piece(q, c):
            at = c * chunk if isinstance(c, int) else pl.multiple_of(c * chunk, rows)
            s = lax.dot_general(
                sk[pl.ds(at, chunk), :], q, (((1,), (1,)), ((), ())), preferred_element_type=F32
            )
            return s, jnp.max(s, axis=0, keepdims=True)

        def softmax(q):
            if keys == chunk:
                s, top = piece(q, 0)
                e = jnp.exp2((s - top) * factor)
                acc = jnp.dot(sv[0], e.astype(BF16), preferred_element_type=F32)
                return acc / jnp.sum(e, axis=0, keepdims=True)

            def step(c, carry):
                old, total, acc = carry
                s, top = piece(q, c)
                top = jnp.maximum(old, top)
                fix = jnp.exp2((old - top) * factor)
                e = jnp.exp2((s - top) * factor)
                acc = acc * fix + jnp.dot(sv[c], e.astype(BF16), preferred_element_type=F32)
                return top, total * fix + jnp.sum(e, axis=0, keepdims=True), acc

            start = (
                jnp.full((1, block), -1e30, F32),
                jnp.zeros((1, block), F32),
                jnp.zeros((vd, block), F32),
            )
            top, total, acc = lax.fori_loop(0, keys // chunk, step, start)
            return acc / total

        for b in range(queries // block):
            q = sq[b * block : (b + 1) * block, :]
            zero = jnp.zeros_like(q)
            first = softmax(jnp.where(lane < half, q, zero))
            second = softmax(jnp.where(lane < half, zero, q))
            ho = first - lam * second
            ho = ho * lax.rsqrt(jnp.mean(ho * ho, axis=0, keepdims=True) + 1e-06)
            so[b * block : (b + 1) * block, :] = (ho.T * gain_ref[...]).astype(BF16)
        for i in range(nq):
            outs[i][...] = so[i * rows : (i + 1) * rows, :]

    return pl.pallas_call(
        body,
        out_shape=[jax.ShapeDtypeStruct((rows, vd), BF16)] * nq,
        in_specs=[SMEM] + [VMEM] * (n + 1),
        out_specs=[VMEM] * nq,
        scratch_shapes=[
            pltpu.VMEM((keys, qk), BF16),
            pltpu.VMEM((keys // chunk, vd, chunk), BF16),
            pltpu.VMEM((queries, qk), BF16),
            pltpu.VMEM((queries, vd), BF16),
        ],
        compiler_params=pltpu.CompilerParams(vmem_limit_bytes=24 << 20),
        name="attend",
    )(mix, gain.reshape(1, vd), *parts)


def project_out(normed, w_out, sharing, masks, rows):
    heads = len(normed)
    total, vd = normed[0].shape

    def body(*refs):
        own_head = lax.axis_index("sp") // sharing
        ins, w, outs, sx = refs[:heads], refs[heads], refs[heads + 1 : -1], refs[-1]
        for j in range(heads):
            h = own_head ^ j
            sx[:, pl.ds(pl.multiple_of(h * vd, vd), vd)] = ins[j][...]
        y = jnp.dot(sx[...], w[...], preferred_element_type=F32)
        for i in range(len(masks)):
            outs[i][...] = y[i * rows : (i + 1) * rows].astype(BF16)

    return pl.pallas_call(
        body,
        out_shape=[jax.ShapeDtypeStruct((rows, w_out.shape[1]), BF16)] * len(masks),
        in_specs=[VMEM] * (heads + 1),
        out_specs=[VMEM] * len(masks),
        scratch_shapes=[pltpu.VMEM((total, heads * vd), BF16)],
        compiler_params=pltpu.CompilerParams(vmem_limit_bytes=12 << 20),
        name="project_out",
    )(*normed, w_out)


def make(n_sp, n_tp):
    def shards(tokens, w_query, w_key, w_value, w_out, mix_weight, out_gain):
        heads = mix_weight.shape[0]
        qk = w_query.shape[1] // heads
        vd = w_value.shape[1] // heads
        rows = tokens.shape[0]
        sharing = n_sp // heads

        weights = (w_key, w_value, w_query)
        bits = []
        while (1 << len(bits)) < n_tp:
            bits.append(1 << len(bits))
        masks, blocks = [0], [tokens]
        for bit in reversed(bits):
            blocks = blocks + [swap(b, "tp", n_tp, bit) for b in blocks]
            masks = masks + [m | bit for m in masks]

        own = project_own(tokens, weights)
        mine = project(own, blocks[1:], weights, heads, sharing)
        q_parts = [mine[0]] + [None] * (heads - 1)
        kv_parts = {}
        relay = heads // 2
        order = ([relay] if relay else []) + [j for j in reversed(range(heads)) if j != relay]
        for j in order:
            if j:
                q_parts[j] = swap(mine[j], "sp", n_sp, j * sharing)
            if not (j and j == relay):
                for r in range(1, sharing):
                    kv_parts[j, r] = swap(mine[heads + j], "sp", n_sp, j * sharing + r)
        if relay:
            for r in range(1, sharing):
                kv_parts[relay, r] = swap(q_parts[relay], "sp", n_sp, r)
        kv_parts = list(kv_parts.values())
        cut = (heads + 1) // 2
        normed = [None] * heads
        for js in (range(cut, heads), range(cut)):
            if not js:
                continue
            rest = [p for j, p in enumerate(q_parts) if j not in js]
            out = attend(
                [q_parts[j] for j in js], rest + kv_parts, mix_weight, out_gain, sharing, qk, vd
            )
            for j, o in zip(js, out):
                normed[j] = swap(o, "sp", n_sp, j * sharing) if j else o
        parts = dict(zip(masks, project_out(normed, w_out, sharing, masks, rows)))
        for bit in bits:
            moved = {m: swap(p, "tp", n_tp, bit) for m, p in parts.items() if m & bit}
            parts = {
                m: (p.astype(F32) + moved[m | bit].astype(F32)).astype(BF16)
                for m, p in parts.items()
                if not m & bit
            }
        return parts[0]

    return shards


def solution(mesh):
    in_specs = (
        P(("sp", "tp"), None),
        P(None, "tp"),
        P(None, "tp"),
        P(None, "tp"),
        P("tp", None),
        P("tp"),
        P(),
    )
    out_specs = P(("sp", "tp"), None)
    inner = make(mesh.shape["sp"], mesh.shape["tp"])

    return jax.shard_map(inner, mesh=mesh, in_specs=in_specs, out_specs=out_specs, check_vma=False)
```
